32 devices in a mesh: sp: 8 (over z, y), tp: 4 (over x, core).
Axes of the slice: x: 2, y: 2, z: 4, core: 2. Of those that a mesh axis runs over, the one named last changes fastest.
Arguments:
- tokens: bfloat16 [2048, 2048], P(('sp', 'tp')), may hold values from -6 to 6
- norm_gain: float32 [2048], replicated, may hold values from 0.1 to 1.9
- ret_query: bfloat16 [2048, 1024], P('sp', 'tp'), may hold values from -0.125 to 0.125
- ret_key: bfloat16 [2048, 1024], P('sp', 'tp'), may hold values from -0.125 to 0.125
- ret_value: bfloat16 [2048, 2048], P('sp', 'tp'), may hold values from -0.125 to 0.125
- log_decay: float32 [8, 2048], P('tp', 'sp'), may hold values from -2 to 0, as said below
- att_query: bfloat16 [2048, 2048], P('sp', 'tp')
- att_key: bfloat16 [2048, 256], P('sp', 'tp')
- att_value: bfloat16 [2048, 256], P('sp', 'tp'), may hold values from -0.125 to 0.125
- sink_logits: float32 [32], P('tp'), may hold values from 3 to 6
- ret_out: bfloat16 [2048, 2048], P('tp', 'sp'), may hold values from -0.125 to 0.125
- att_out: bfloat16 [2048, 2048], P('tp', 'sp'), may hold values from -1 to 1
Outputs:
- mixed: bfloat16 [2048, 2048], P(('sp', 'tp'))
The draws below stay inside these ranges and needn't reach their ends.
Inputs may be any that keep to these rules, and one draw needn't show every extreme that they name: `log_decay`: strictly negative.
All inputs are finite; a program needn't handle non-finite values.
Results may differ from the reference program's by a relative error of at most 0.013.
Values may be sent and summed in bfloat16 or wider, within the bound.
A program may use at most 128 MiB of HBM per device.

```python
import jax
import jax.numpy as jnp
from jax import lax

D = 2048
RET_HEADS = 8
RETAIN_KEY_SIZE = 128
V_DIM = 256
ASKER_HEADCOUNT = 32
KV_HEADS = 4
HEAD_DIM = 64
WINDOW = 128
BLOCK = 128
TOKENS = 2048
N_TP = 4


def attend_pair(key):
    lookup_matrix = jax.random.normal(jax.random.fold_in(key, 11), (D, KV_HEADS * HEAD_DIM), jnp.float32) * D ** (-0.5)
    query_weight = jax.random.normal(jax.random.fold_in(key, 12), (D, ASKER_HEADCOUNT * HEAD_DIM), jnp.float32) * D ** (-0.5)
    return (query_weight, lookup_matrix)


def draw_att_query(key, part):
    return attend_pair(key)[0].astype(jnp.bfloat16)


def draw_att_key(key, part):
    return attend_pair(key)[1].astype(jnp.bfloat16)


def draw_log_decay(key, part):
    slow_share = 0.5
    picked = jax.random.uniform(jax.random.fold_in(key, 21), (RET_HEADS,))
    fast_rate = jax.random.uniform(jax.random.fold_in(key, 22), (RET_HEADS,), minval=1.0 / 100.0, maxval=1.0 / 30.0)
    slow_rate = jax.random.uniform(jax.random.fold_in(key, 23), (RET_HEADS,), minval=0.2, maxval=0.6) / TOKENS
    speed_numbers = jnp.where(picked < slow_share, slow_rate, fast_rate)
    tempo_numbers = jax.random.uniform(jax.random.fold_in(key, 24), (TOKENS // BLOCK,), minval=0.6, maxval=1.5)
    tempo_numbers = jnp.repeat(tempo_numbers, BLOCK)
    spots = jax.random.randint(jax.random.fold_in(key, 25), (RET_HEADS, 2), 0, TOKENS)
    objective_numbers = jnp.log(jax.random.uniform(jax.random.fold_in(key, 26), (RET_HEADS, 2), minval=0.5, maxval=0.8))
    removed_elements = jnp.arange(TOKENS)[None, None, :] == spots[:, :, None]
    spike_sequence = jnp.sum(jnp.where(removed_elements, objective_numbers[:, :, None], 0.0), axis=1)
    return -speed_numbers[:, None] * tempo_numbers[None, :] + spike_sequence


def shard_levels(own_key, extent, pieces, least, top_value):
    def one(position, shards_of):
        steps = jax.random.uniform(jax.random.fold_in(jax.random.fold_in(own_key, 6), position), (shards_of,), jnp.float32, least / len(pieces), top_value / len(pieces))
        return jnp.repeat(jnp.exp(steps), extent[position] // shards_of).reshape((-1,) + (1,) * (len(extent) - position - 1))

    gain = one(*pieces[0])
    for cut in pieces[1:]:
        gain = gain * one(*cut)
    return gain


def centred(rng, shape, deviation, bound, shards=(), kind=jnp.bfloat16):
    factor_of = shard_levels(rng, shape, shards, -0.22, 0.18) if shards else 1.0
    result = jax.random.normal(rng, shape, jnp.float32) * deviation * factor_of
    return jnp.minimum(jnp.maximum(result, -bound), bound).astype(kind)


def setup_inputs(seed: int = 0) -> dict:
    seeds = jax.random.split(jax.random.key(seed), 13)
    return {
        "tokens": centred(seeds[0], (TOKENS, D), 1.0, 6.0, ((0, 32),)),
        "norm_gain": jnp.clip(1.0 + 0.18 * jax.random.normal(seeds[1], (D,), jnp.float32), 0.1, 1.9),
        "ret_query": centred(seeds[2], (D, RET_HEADS * RETAIN_KEY_SIZE), D ** -0.5, 0.125, ((0, 8), (1, 4))),
        "ret_key": centred(seeds[3], (D, RET_HEADS * RETAIN_KEY_SIZE), D ** -0.5, 0.125, ((0, 8), (1, 4))),
        "ret_value": centred(seeds[4], (D, RET_HEADS * V_DIM), D ** -0.5, 0.125, ((0, 8), (1, 4))),
        "log_decay": draw_log_decay(jax.random.fold_in(seeds[12], 71), 0),
        "att_query": draw_att_query(jax.random.fold_in(seeds[12], 71), 0),
        "att_key": draw_att_key(jax.random.fold_in(seeds[12], 71), 0),
        "att_value": centred(seeds[8], (D, KV_HEADS * HEAD_DIM), D ** -0.5, 0.125, ((0, 8), (1, 4))),
        "sink_logits": jnp.clip(3.0 + 3.0 * jax.random.uniform(seeds[9], (ASKER_HEADCOUNT,), jnp.float32) ** shard_levels(seeds[9], (ASKER_HEADCOUNT,), ((0, 4),), -0.2, 0.2), 3.0, 6.0),
        "ret_out": centred(seeds[10], (RET_HEADS * V_DIM, D), (RET_HEADS * V_DIM) ** -0.5, 0.125, ((0, 4), (1, 8))),
        "att_out": centred(seeds[11], (ASKER_HEADCOUNT * HEAD_DIM, D), (ASKER_HEADCOUNT * HEAD_DIM // 64) ** -0.5, 1.0, ((0, 4), (1, 8))),
    }


epsilon = 1e-05
rope_base = 10000.0
masked_out = -1e+30

def rounded(values):
    return lax.optimization_barrier(values.astype(jnp.bfloat16))

def rotate(values, positions):
    half_dim = values.shape[-1] // 2
    inverse = rope_base ** (-jnp.arange(half_dim, dtype=jnp.float32) / half_dim)
    angles = positions.astype(jnp.float32)[:, None] * inverse[None, :]
    cosine = jnp.cos(angles)[:, None, :]
    sine_part = jnp.sin(angles)[:, None, :]
    first_half = values[..., :half_dim].astype(jnp.float32)
    second_half = values[..., half_dim:].astype(jnp.float32)
    return jnp.concatenate([first_half * cosine - second_half * sine_part, second_half * cosine + first_half * sine_part], axis=-1)

def retain(query, keys, values, log_decay):
    length, head_count, key_depth = query.shape
    value_width = values.shape[-1]
    block_count = length // BLOCK
    q_blocks = query.reshape(block_count, BLOCK, head_count, key_depth).astype(jnp.float32)
    k_blocks = keys.reshape(block_count, BLOCK, head_count, key_depth).astype(jnp.float32)
    v_blocks = values.reshape(block_count, BLOCK, head_count, value_width).astype(jnp.float32)
    running = jnp.cumsum(log_decay.reshape(head_count, block_count, BLOCK), axis=-1)
    closing = running[:, :, -1:]
    within = running[:, :, :, None] - running[:, :, None, :]
    causal_mask = jnp.arange(BLOCK)[:, None] >= jnp.arange(BLOCK)[None, :]
    weighting = jnp.where(causal_mask, jnp.exp(jnp.minimum(within, 0.0)), 0.0)
    scores = jnp.einsum('nihd,njhd->hnij', q_blocks, k_blocks) * weighting
    in_block = jnp.einsum('hnij,njhv->nihv', rounded(scores).astype(jnp.float32), v_blocks)
    key_fade = rounded(k_blocks * jnp.exp(closing - running).transpose(1, 2, 0)[..., None])
    contrib = jnp.einsum('njhd,njhv->nhdv', key_fade.astype(jnp.float32), v_blocks)
    block_fade = jnp.exp(closing[:, :, 0]).T

    def advance(carried, entry_pair):
        addend, factor = entry_pair
        return (carried * factor[:, None, None] + addend, carried)
    _, before = lax.scan(advance, jnp.zeros((head_count, key_depth, value_width), jnp.float32), (contrib, block_fade))
    query_fade = rounded(q_blocks * jnp.exp(running).transpose(1, 2, 0)[..., None])
    carried_term = jnp.einsum('nihd,nhdv->nihv', query_fade.astype(jnp.float32), before, precision=lax.Precision.HIGHEST)
    final_product = in_block + carried_term
    final_product = final_product * lax.rsqrt(lax.optimization_barrier(jnp.mean(final_product * final_product, axis=-1, keepdims=True)) + epsilon)
    return final_product.reshape(length, head_count * value_width).astype(jnp.bfloat16)

def one_group(group_entry):
    queries, keys, values, sink_row = group_entry
    length = keys.shape[0]
    group_size = queries.shape[1]
    block_count = length // WINDOW
    zeroed = jnp.zeros((WINDOW, HEAD_DIM), jnp.bfloat16)
    key_ext = jnp.concatenate([zeroed, keys], axis=0).reshape(block_count + 1, WINDOW, HEAD_DIM)
    value_ext = jnp.concatenate([zeroed, values], axis=0).reshape(block_count + 1, WINDOW, HEAD_DIM)
    keys_pair = jnp.concatenate([key_ext[:-1], key_ext[1:]], axis=1).astype(jnp.float32)
    values_pair = jnp.concatenate([value_ext[:-1], value_ext[1:]], axis=1).astype(jnp.float32)
    q_blocks = queries.reshape(block_count, WINDOW, group_size, HEAD_DIM).astype(jnp.float32)
    scores = jnp.einsum('nigd,njd->ngij', q_blocks, keys_pair) * HEAD_DIM ** (-0.5)
    query_pos = (jnp.arange(block_count) * WINDOW)[:, None] + jnp.arange(WINDOW)[None, :]
    key_pos = (jnp.arange(block_count) * WINDOW - WINDOW)[:, None] + jnp.arange(2 * WINDOW)[None, :]
    allowed = (key_pos[:, None, :] >= 0) & (key_pos[:, None, :] <= query_pos[:, :, None]) & (query_pos[:, :, None] - key_pos[:, None, :] < WINDOW)
    scores = jnp.where(allowed[:, None], scores, masked_out)
    sink_logit = sink_row[None, :, None]
    highest = jnp.maximum(lax.optimization_barrier(jnp.max(scores, axis=-1)), sink_logit)
    lifted = jnp.exp(scores - highest[..., None])
    denominator = lax.optimization_barrier(jnp.sum(lifted, axis=-1)) + jnp.exp(sink_logit - highest)
    attn_weights = rounded(lifted / denominator[..., None])
    final_product = jnp.einsum('ngij,njd->nigd', attn_weights.astype(jnp.float32), values_pair)
    return final_product.reshape(length, group_size * HEAD_DIM).astype(jnp.bfloat16)

def reference(tokens, norm_gain, ret_query, ret_key, ret_value, log_decay, att_query, att_key, att_value, sink_logits, ret_out, att_out):
    tok_float = tokens.astype(jnp.float32)
    normed = (tok_float * lax.rsqrt(lax.optimization_barrier(jnp.mean(tok_float * tok_float, axis=-1, keepdims=True)) + epsilon) * norm_gain).astype(jnp.bfloat16)

    def project(weight):
        return jnp.dot(normed, weight, preferred_element_type=jnp.float32).astype(jnp.bfloat16)
    positions = jnp.arange(TOKENS, dtype=jnp.int32)
    query_ret = rotate(project(ret_query).reshape(TOKENS, RET_HEADS, RETAIN_KEY_SIZE), positions).astype(jnp.bfloat16)
    key_ret = (rotate(project(ret_key).reshape(TOKENS, RET_HEADS, RETAIN_KEY_SIZE), positions) * RETAIN_KEY_SIZE ** (-0.5)).astype(jnp.bfloat16)
    value_ret = project(ret_value).reshape(TOKENS, RET_HEADS, V_DIM)
    ret_mix = retain(query_ret, key_ret, value_ret, log_decay)
    group_size = ASKER_HEADCOUNT // KV_HEADS
    query_att = project(att_query).reshape(TOKENS, KV_HEADS, group_size, HEAD_DIM).transpose(1, 0, 2, 3)
    key_att = project(att_key).reshape(TOKENS, KV_HEADS, HEAD_DIM).transpose(1, 0, 2)
    value_att = project(att_value).reshape(TOKENS, KV_HEADS, HEAD_DIM).transpose(1, 0, 2)
    att_mix = lax.map(one_group, (query_att, key_att, value_att, sink_logits.reshape(KV_HEADS, group_size)))
    att_mix = att_mix.transpose(1, 0, 2).reshape(TOKENS, ASKER_HEADCOUNT * HEAD_DIM)
    ret_share = RET_HEADS * V_DIM // N_TP
    att_share = ASKER_HEADCOUNT * HEAD_DIM // N_TP
    summed = jnp.zeros((TOKENS, D), jnp.float32)
    for group_index in range(N_TP):
        ret_cols = slice(group_index * ret_share, (group_index + 1) * ret_share)
        att_cols = slice(group_index * att_share, (group_index + 1) * att_share)
        partial_total_sum = jnp.dot(ret_mix[:, ret_cols], ret_out[ret_cols], preferred_element_type=jnp.float32)
        partial_total_sum = partial_total_sum + jnp.dot(att_mix[:, att_cols], att_out[att_cols], preferred_element_type=jnp.float32)
        summed = summed + rounded(partial_total_sum).astype(jnp.float32)
    return summed.astype(jnp.bfloat16)
```

```python
import functools

import jax
import jax.numpy as jnp
from jax import lax
from jax.experimental import pallas as pl
from jax.experimental.pallas import tpu as pltpu
from jax.sharding import PartitionSpec as P

MESH = pl.DeviceIdType.MESH
LANES = 128

RETAIN_KEY_SIZE = 128
V_DIM = 256
HEAD_DIM = 64
WINDOW = 128
BLOCK = 128


epsilon = 1e-05
rope_base = 10000.0
masked_out = -1e30


def prefix(part, axis, combine, identity):
    place = lax.axis_index(axis)
    gathered = jax.tree.map(lambda a: lax.all_gather(a, axis), part)
    state = jax.tree.map(lambda a, e: jnp.zeros_like(a) + jnp.asarray(e, a.dtype), part, identity)

    def one(lap, state):
        return combine(
            state, jax.tree.map(lambda a: lax.dynamic_index_in_dim(a, lap, 0, False), gathered)
        )

    return lax.fori_loop(0, place, one, state)


def shifted(value, axis, steps):
    count = lax.axis_size(axis)
    initial, last = (max(0, -steps), min(count, count - steps))
    return lax.ppermute(value, axis, [(source, source + steps) for source in range(initial, last)])


def rotate(values, positions):
    half_dim = values.shape[-1] // 2
    inverse = rope_base ** (-jnp.arange(half_dim, dtype=jnp.float32) / half_dim)
    angles = positions.astype(jnp.float32)[:, None] * inverse[None, :]
    cosine = jnp.cos(angles)[:, None, :]
    sine_part = jnp.sin(angles)[:, None, :]
    first_half = values[..., :half_dim].astype(jnp.float32)
    second_half = values[..., half_dim:].astype(jnp.float32)
    return jnp.concatenate(
        [
            first_half * cosine - second_half * sine_part,
            second_half * cosine + first_half * sine_part,
        ],
        axis=-1,
    )


def chain_join(earlier_part, later_part):
    return (
        earlier_part[0] * later_part[0],
        later_part[0][:, None, None] * earlier_part[1] + later_part[1],
    )


def retention_path(query_ret, key_ret, value_ret, log_decay):
    tok_count, heads_here = (query_ret.shape[0], query_ret.shape[1])
    blocks = tok_count // BLOCK
    q_blocks = query_ret.reshape(blocks, BLOCK, heads_here, RETAIN_KEY_SIZE)
    k_blocks = key_ret.reshape(blocks, BLOCK, heads_here, RETAIN_KEY_SIZE)
    v_blocks = value_ret.reshape(blocks, BLOCK, heads_here, V_DIM)
    running = jnp.cumsum(log_decay.reshape(heads_here, blocks, BLOCK), axis=-1)
    closing = running[:, :, -1:]
    within = running[:, :, :, None] - running[:, :, None, :]
    causal_mask = jnp.arange(BLOCK)[:, None] >= jnp.arange(BLOCK)[None, :]
    weighting = jnp.where(causal_mask, jnp.exp(jnp.minimum(within, 0.0)), 0.0)
    scores = (
        jnp.einsum("nihd,njhd->hnij", q_blocks, k_blocks, preferred_element_type=jnp.float32)
        * weighting
    )
    in_block = jnp.einsum(
        "hnij,njhv->nihv", scores.astype(jnp.bfloat16), v_blocks, preferred_element_type=jnp.float32
    )
    key_fade = (
        k_blocks.astype(jnp.float32) * jnp.exp(closing - running).transpose(1, 2, 0)[..., None]
    ).astype(jnp.bfloat16)
    contrib = jnp.einsum("njhd,njhv->nhdv", key_fade, v_blocks, preferred_element_type=jnp.float32)
    block_fade = jnp.exp(closing[:, :, 0]).T

    def advance(carried, entry_pair):
        addend, factor = entry_pair
        return (carried * factor[:, None, None] + addend, carried)

    final_state, before = lax.scan(
        advance, jnp.zeros((heads_here, RETAIN_KEY_SIZE, V_DIM), jnp.float32), (contrib, block_fade)
    )
    device_fade = jnp.exp(jnp.sum(closing[:, :, 0], axis=1))
    identity = (jnp.ones_like(device_fade), jnp.zeros_like(final_state))
    arrived = prefix((device_fade, final_state), "sp", chain_join, identity)
    leading = jnp.cumsum(closing[:, :, 0], axis=1) - closing[:, :, 0]
    before = before + arrived[1][None] * jnp.exp(leading).T[:, :, None, None]
    query_fade = (
        q_blocks.astype(jnp.float32) * jnp.exp(running).transpose(1, 2, 0)[..., None]
    ).astype(jnp.bfloat16)
    carried_term = jnp.einsum(
        "nihd,nhdv->nihv", query_fade.astype(jnp.float32), before, precision=lax.Precision.HIGHEST
    )
    final_product = in_block + carried_term
    final_product = final_product * lax.rsqrt(
        jnp.mean(final_product * final_product, axis=-1, keepdims=True) + epsilon
    )
    return final_product.reshape(tok_count, heads_here * V_DIM).astype(jnp.bfloat16)


def attention_path(query_att, key_att, value_att, sink_logits, anchor):
    tok_count = query_att.shape[0]
    kv_here = key_att.shape[1] // HEAD_DIM
    group_size = query_att.shape[1] // (kv_here * HEAD_DIM)
    stacked = jnp.concatenate([key_att, value_att], axis=1)
    window_rim = shifted(stacked[tok_count - WINDOW :], "sp", 1)
    blocks = tok_count // WINDOW
    extended = jnp.concatenate([window_rim, stacked], axis=0).reshape(
        blocks + 1, WINDOW, 2, kv_here, HEAD_DIM
    )
    paired = jnp.concatenate([extended[:-1], extended[1:]], axis=1)
    keys_pair = paired[:, :, 0]
    values_pair = paired[:, :, 1]
    q_blocks = query_att.reshape(blocks, WINDOW, kv_here, group_size, HEAD_DIM)
    scores = jnp.einsum(
        "nihgd,njhd->nhgij", q_blocks, keys_pair, preferred_element_type=jnp.float32
    ) * HEAD_DIM ** (-0.5)
    query_pos = anchor + (jnp.arange(blocks) * WINDOW)[:, None] + jnp.arange(WINDOW)[None, :]
    key_pos = (
        anchor + (jnp.arange(blocks) * WINDOW - WINDOW)[:, None] + jnp.arange(2 * WINDOW)[None, :]
    )
    allowed = (
        (key_pos[:, None, :] >= 0)
        & (key_pos[:, None, :] <= query_pos[:, :, None])
        & (query_pos[:, :, None] - key_pos[:, None, :] < WINDOW)
    )
    scores = jnp.where(allowed[:, None, None], scores, masked_out)
    sink_logit = sink_logits.reshape(kv_here, group_size)[None, :, :, None]
    highest = jnp.maximum(jnp.max(scores, axis=-1), sink_logit)
    lifted = jnp.exp(scores - highest[..., None])
    denominator = jnp.sum(lifted, axis=-1) + jnp.exp(sink_logit - highest)
    attn_weights = (lifted / denominator[..., None]).astype(jnp.bfloat16)
    final_product = jnp.einsum(
        "nhgij,njhd->nihgd", attn_weights, values_pair, preferred_element_type=jnp.float32
    )
    return final_product.reshape(tok_count, kv_here * group_size * HEAD_DIM).astype(jnp.bfloat16)


def ring_spot(index, count):
    half = count // 2
    return jnp.where(lax.rem(index, 2) == 0, index // 2, count - 1 - index // 2)


def ring_member(spot, count):
    half = count // 2
    return jnp.where(spot < half, 2 * spot, 2 * (count - 1 - spot) + 1)


def project_kernel(n, n_tp, normed_ref, pack_ref, out_ref, rows_ref, held, total, sems, tok_sems):
    sp, tp = lax.axis_index("sp"), lax.axis_index("tp")
    depth, width = pack_ref.shape
    count = normed_ref.shape[0]
    half = n // 2
    spot = ring_spot(sp, n)
    ahead = ring_member(lax.rem(spot + 1, n), n)
    behind = ring_member(lax.rem(spot + n - 1, n), n)

    barrier = pltpu.get_barrier_semaphore()
    for peer in (ahead, behind):
        pl.semaphore_signal(barrier, inc=1, device_id=(peer, tp), device_id_type=MESH)
    for step in range(1, n_tp):
        pl.semaphore_signal(
            barrier, inc=1, device_id=(sp, lax.rem(tp + step, n_tp)), device_id_type=MESH
        )
    pl.semaphore_wait(barrier, 2 + n_tp - 1)

    def rows_of(member):
        return pl.ds(pl.multiple_of(member * depth, depth), depth)

    middle = (width // LANES + 1) // 2 * LANES
    spans = (pl.ds(0, middle), pl.ds(middle, width - middle))

    def owner(direction, distance):
        shift = n - distance if direction == 0 else distance
        return ring_member(lax.rem(spot + shift, n), n)

    def send(direction, step, part):
        member = owner(direction, step - 1)
        source = pack_ref.at[:, spans[part]] if step == 1 else held.at[rows_of(member), spans[part]]
        return pltpu.make_async_remote_copy(
            src_ref=source,
            dst_ref=held.at[rows_of(member), spans[part]],
            send_sem=sems.at[0, direction, step - 1, part],
            recv_sem=sems.at[1, direction, step - 1, part],
            device_id=(ahead if direction == 0 else behind, tp),
            device_id_type=MESH,
        )

    def arrival(direction, step, part):
        member = owner(direction, step)
        return pltpu.make_async_remote_copy(
            src_ref=held.at[rows_of(member), spans[part]],
            dst_ref=held.at[rows_of(member), spans[part]],
            send_sem=sems.at[0, direction, step - 1, part],
            recv_sem=sems.at[1, direction, step - 1, part],
            device_id=(ahead if direction == 0 else behind, tp),
            device_id_type=MESH,
        )

    started = []

    def go(copy):
        copy.start()
        started.append(copy)

    def parts_of(step, direction):
        first = direction
        return (first,) if step == half else (first, 1 - first)

    for slot in range(2):
        for direction in range(2):
            parts = parts_of(1, direction)
            if slot < len(parts):
                go(send(direction, 1, parts[slot]))
    tok_here = pl.ds(pl.multiple_of(tp * count, count), count)
    for step in range(1, n_tp):
        go(
            pltpu.make_async_remote_copy(
                src_ref=normed_ref,
                dst_ref=rows_ref.at[tok_here],
                send_sem=tok_sems.at[0, step - 1],
                recv_sem=tok_sems.at[1, step - 1],
                device_id=(sp, lax.rem(tp + step, n_tp)),
                device_id_type=MESH,
            )
        )
    rows_ref[tok_here, :] = normed_ref[...]
    for step in range(1, n_tp):
        origin = pl.ds(pl.multiple_of(lax.rem(tp + n_tp - step, n_tp) * count, count), count)
        pltpu.make_async_remote_copy(
            src_ref=normed_ref,
            dst_ref=rows_ref.at[origin],
            send_sem=tok_sems.at[0, step - 1],
            recv_sem=tok_sems.at[1, step - 1],
            device_id=(sp, lax.rem(tp + step, n_tp)),
            device_id_type=MESH,
        ).wait_recv()

    blockwise = depth % LANES == 0

    def add(member, weights, first=False):
        columns = pl.ds(pl.multiple_of(member * depth, depth), depth)
        product = jnp.dot(rows_ref[:, columns], weights, preferred_element_type=jnp.float32)
        total[...] = product if first else total[...] + product

    if blockwise:
        add(sp, pack_ref[...], True)
    else:
        held[rows_of(sp), :] = pack_ref[...]
    for step in range(1, half + 1):
        for slot in range(2):
            for direction in range(2):
                parts = parts_of(step, direction)
                if slot < len(parts):
                    arrival(direction, step, parts[slot]).wait_recv()
                    if step < half and parts[slot] in parts_of(step + 1, direction):
                        go(send(direction, step + 1, parts[slot]))
        if blockwise:
            for direction in range(1 if step == half else 2):
                member = owner(direction, step)
                add(member, held[rows_of(member), :])
    if not blockwise:
        total[...] = jnp.dot(rows_ref[...], held[...], preferred_element_type=jnp.float32)
    out_ref[...] = total[...].astype(out_ref.dtype)
    for copy in started:
        copy.wait_send()


def project(normed, pack, n, n_tp):
    depth, width = pack.shape
    count = normed.shape[0]
    features = normed.shape[1]
    vmem = pl.BlockSpec(memory_space=pltpu.VMEM)
    return pl.pallas_call(
        functools.partial(project_kernel, n, n_tp),
        out_shape=jax.ShapeDtypeStruct((n_tp * count, width), jnp.bfloat16),
        in_specs=[vmem, vmem],
        out_specs=vmem,
        scratch_shapes=[
            pltpu.VMEM((n_tp * count, features), jnp.bfloat16),
            pltpu.VMEM((n * depth, width), jnp.bfloat16),
            pltpu.VMEM((n_tp * count, width), jnp.float32),
            pltpu.SemaphoreType.DMA((2, 2, n // 2, 2)),
            pltpu.SemaphoreType.DMA((2, n_tp - 1)),
        ],
        compiler_params=pltpu.CompilerParams(
            collective_id=0, has_side_effects=True, vmem_limit_bytes=40 * 2**20
        ),
        cost_estimate=pl.CostEstimate(
            flops=400 * 2**30, bytes_accessed=n * depth * width * 2, transcendentals=0
        ),
        name="project_ring",
    )(normed, pack)


def merge_kernel(n_tp, mix_ref, weight_ref, out_ref, outgoing, incoming, sent, landed, sems):
    sp, tp = lax.axis_index("sp"), lax.axis_index("tp")
    outer, inner = tp // 2, lax.rem(tp, 2)
    groups = n_tp // 2
    count = out_ref.shape[0]
    barrier = pltpu.get_barrier_semaphore()
    mate = outer * 2 + 1 - inner
    pl.semaphore_signal(barrier, inc=1, device_id=(sp, mate), device_id_type=MESH)
    for step in range(1, groups):
        peer = lax.rem(outer + step, groups) * 2 + inner
        pl.semaphore_signal(barrier, inc=1, device_id=(sp, peer), device_id_type=MESH)
    pl.semaphore_wait(barrier, groups)

    outgoing[...] = jnp.dot(
        mix_ref[1 - inner], weight_ref[...], preferred_element_type=jnp.float32
    ).astype(jnp.bfloat16)
    swap = pltpu.make_async_remote_copy(
        src_ref=outgoing,
        dst_ref=incoming,
        send_sem=sems.at[0, 0],
        recv_sem=sems.at[1, 0],
        device_id=(sp, mate),
        device_id_type=MESH,
    )
    swap.start()
    own = jnp.dot(mix_ref[inner], weight_ref[...], preferred_element_type=jnp.float32)
    swap.wait_recv()
    own = own + incoming[...].astype(jnp.float32)
    sent[...] = own.astype(jnp.bfloat16)
    copies = []
    for step in range(1, groups):
        other = lax.rem(outer + step, groups)
        copy = pltpu.make_async_remote_copy(
            src_ref=sent.at[pl.ds(pl.multiple_of(other * count, count), count)],
            dst_ref=landed.at[step - 1],
            send_sem=sems.at[0, step],
            recv_sem=sems.at[1, step],
            device_id=(sp, other * 2 + inner),
            device_id_type=MESH,
        )
        copy.start()
        copies.append(copy)
    mine = sent[pl.ds(pl.multiple_of(outer * count, count), count), :].astype(jnp.float32)
    for step, copy in enumerate(copies):
        copy.wait_recv()
        mine = mine + landed[step].astype(jnp.float32)
    out_ref[...] = mine.astype(out_ref.dtype)
    swap.wait_send()
    for copy in copies:
        copy.wait_send()


def merge(mix, weight, n_tp):
    rows = mix.shape[0]
    groups = n_tp // 2
    count = rows // n_tp
    width = weight.shape[1]
    mix = mix.reshape(groups, 2, count, mix.shape[1]).transpose(1, 0, 2, 3)
    mix = mix.reshape(2, groups * count, -1)
    vmem = pl.BlockSpec(memory_space=pltpu.VMEM)
    return pl.pallas_call(
        functools.partial(merge_kernel, n_tp),
        out_shape=jax.ShapeDtypeStruct((count, width), jnp.bfloat16),
        in_specs=[vmem, vmem],
        out_specs=vmem,
        scratch_shapes=[
            pltpu.VMEM((groups * count, width), jnp.bfloat16),
            pltpu.VMEM((groups * count, width), jnp.bfloat16),
            pltpu.VMEM((groups * count, width), jnp.bfloat16),
            pltpu.VMEM((max(1, groups - 1), count, width), jnp.bfloat16),
            pltpu.SemaphoreType.DMA((2, groups)),
        ],
        compiler_params=pltpu.CompilerParams(
            collective_id=1, has_side_effects=True, vmem_limit_bytes=40 * 2**20
        ),
        cost_estimate=pl.CostEstimate(
            flops=2 * rows * weight.shape[0] * width, bytes_accessed=2 * weight.size, transcendentals=0
        ),
        name="merge_scatter",
    )(mix, weight)


def on_device(
    tokens,
    norm_gain,
    ret_query,
    ret_key,
    ret_value,
    log_decay,
    att_query,
    att_key,
    att_value,
    sink_logits,
    ret_out,
    att_out,
):
    tok_float = tokens.astype(jnp.float32)
    normed = (
        tok_float
        * lax.rsqrt(jnp.mean(tok_float * tok_float, axis=-1, keepdims=True) + epsilon)
        * norm_gain
    ).astype(jnp.bfloat16)
    n, n_tp = lax.axis_size("sp"), lax.axis_size("tp")
    weights = (ret_query, ret_key, ret_value, att_query, att_key, att_value)
    widths = [weight.shape[1] for weight in weights]
    points = [sum(widths[:index]) for index in range(1, len(widths))]
    out_whole = lax.all_gather(jnp.concatenate([ret_out, att_out], axis=0), "sp", axis=1, tiled=True)
    projected = project(normed, jnp.concatenate(weights, axis=1), n, n_tp)
    sections = jnp.split(projected, points, axis=1)
    tok_count = sections[0].shape[0]
    anchor = lax.axis_index("sp") * tok_count
    positions = anchor + jnp.arange(tok_count, dtype=jnp.int32)
    query_ret = rotate(sections[0].reshape(tok_count, -1, RETAIN_KEY_SIZE), positions).astype(
        jnp.bfloat16
    )
    key_ret = (
        rotate(sections[1].reshape(tok_count, -1, RETAIN_KEY_SIZE), positions)
        * RETAIN_KEY_SIZE ** (-0.5)
    ).astype(jnp.bfloat16)
    value_ret = sections[2].reshape(tok_count, -1, V_DIM)
    ret_mix = retention_path(query_ret, key_ret, value_ret, log_decay)
    att_mix = attention_path(sections[3], sections[4], sections[5], sink_logits, anchor)
    return merge(jnp.concatenate([ret_mix, att_mix], axis=1), out_whole, n_tp)


def solution(mesh):
    in_specs = (
        P(("sp", "tp"), None),
        P(),
        P("sp", "tp"),
        P("sp", "tp"),
        P("sp", "tp"),
        P("tp", "sp"),
        P("sp", "tp"),
        P("sp", "tp"),
        P("sp", "tp"),
        P("tp"),
        P("tp", "sp"),
        P("tp", "sp"),
    )
    out_specs = P(("sp", "tp"), None)
    return jax.shard_map(
        on_device, mesh=mesh, in_specs=in_specs, out_specs=out_specs, check_vma=False
    )
```

```python
import functools

import jax
import jax.numpy as jnp
from jax import lax
from jax.experimental import pallas as pl
from jax.experimental.pallas import tpu as pltpu
from jax.sharding import PartitionSpec as P

MESH = pl.DeviceIdType.MESH
LANES = 128

RETAIN_KEY_SIZE = 128
V_DIM = 256
HEAD_DIM = 64
WINDOW = 128
BLOCK = 128


epsilon = 1e-05
rope_base = 10000.0
masked_out = -1e30


def rotate(values, positions):
    half_dim = values.shape[-1] // 2
    inverse = rope_base ** (-jnp.arange(half_dim, dtype=jnp.float32) / half_dim)
    angles = positions.astype(jnp.float32)[:, None] * inverse[None, :]
    cosine = jnp.cos(angles)[:, None, :]
    sine_part = jnp.sin(angles)[:, None, :]
    first_half = values[..., :half_dim].astype(jnp.float32)
    second_half = values[..., half_dim:].astype(jnp.float32)
    return jnp.concatenate(
        [
            first_half * cosine - second_half * sine_part,
            second_half * cosine + first_half * sine_part,
        ],
        axis=-1,
    )


def retention_path(query_ret, key_ret, value_ret, log_decay, rim, logs, weights):
    tok_count, heads_here = (query_ret.shape[0], query_ret.shape[1])
    blocks = tok_count // BLOCK
    q_blocks = query_ret.reshape(blocks, BLOCK, heads_here, RETAIN_KEY_SIZE)
    k_blocks = key_ret.reshape(blocks, BLOCK, heads_here, RETAIN_KEY_SIZE)
    v_blocks = value_ret.reshape(blocks, BLOCK, heads_here, V_DIM)
    running = jnp.cumsum(log_decay.reshape(heads_here, blocks, BLOCK), axis=-1)
    closing = running[:, :, -1:]
    within = running[:, :, :, None] - running[:, :, None, :]
    causal_mask = jnp.arange(BLOCK)[:, None] >= jnp.arange(BLOCK)[None, :]
    weighting = jnp.where(causal_mask, jnp.exp(jnp.minimum(within, 0.0)), 0.0)
    scores = (
        jnp.einsum("nihd,njhd->hnij", q_blocks, k_blocks, preferred_element_type=jnp.float32)
        * weighting
    )
    in_block = jnp.einsum(
        "hnij,njhv->nihv", scores.astype(jnp.bfloat16), v_blocks, preferred_element_type=jnp.float32
    )
    key_fade = (
        k_blocks.astype(jnp.float32) * jnp.exp(closing - running).transpose(1, 2, 0)[..., None]
    ).astype(jnp.bfloat16)
    contrib = jnp.einsum("njhd,njhv->nhdv", key_fade, v_blocks, preferred_element_type=jnp.float32)
    block_fade = jnp.exp(closing[:, :, 0]).T

    def advance(carried, entry_pair):
        addend, factor = entry_pair
        return (carried * factor[:, None, None] + addend, carried)

    final_state, before = lax.scan(
        advance, jnp.zeros((heads_here, RETAIN_KEY_SIZE, V_DIM), jnp.float32), (contrib, block_fade)
    )
    n = lax.axis_size("sp")
    place = lax.axis_index("sp")
    before_rim, states, *wholes = exchange(
        rim, final_state.astype(jnp.bfloat16).reshape(2, -1, V_DIM), weights, n
    )
    states = states.reshape(n, heads_here, RETAIN_KEY_SIZE, V_DIM)
    spots = jnp.arange(n)
    between = (spots[None, :] > spots[:, None]) & (spots[None, :] < place)
    spans = jnp.sum(jnp.where(between[:, :, None], logs[None], 0.0), axis=1)
    shares = jnp.where((spots < place)[:, None], jnp.exp(spans), 0.0)
    arrived = jnp.sum(shares[:, :, None, None] * states.astype(jnp.float32), axis=0)
    leading = jnp.cumsum(closing[:, :, 0], axis=1) - closing[:, :, 0]
    before = before + arrived[None] * jnp.exp(leading).T[:, :, None, None]
    query_fade = (
        q_blocks.astype(jnp.float32) * jnp.exp(running).transpose(1, 2, 0)[..., None]
    ).astype(jnp.bfloat16)
    carried_term = jnp.einsum(
        "nihd,nhdv->nihv", query_fade.astype(jnp.float32), before, precision=lax.Precision.HIGHEST
    )
    final_product = in_block + carried_term
    final_product = final_product * lax.rsqrt(
        jnp.mean(final_product * final_product, axis=-1, keepdims=True) + epsilon
    )
    return final_product.reshape(tok_count, heads_here * V_DIM).astype(jnp.bfloat16), before_rim, wholes


def attention_path(query_att, stacked, window_rim, sink_logits, anchor):
    tok_count = query_att.shape[0]
    kv_here = stacked.shape[1] // (2 * HEAD_DIM)
    group_size = query_att.shape[1] // (kv_here * HEAD_DIM)
    blocks = tok_count // WINDOW
    extended = jnp.concatenate([window_rim, stacked], axis=0).reshape(
        blocks + 1, WINDOW, 2, kv_here, HEAD_DIM
    )
    paired = jnp.concatenate([extended[:-1], extended[1:]], axis=1)
    keys_pair = paired[:, :, 0]
    values_pair = paired[:, :, 1]
    q_blocks = query_att.reshape(blocks, WINDOW, kv_here, group_size, HEAD_DIM)
    scores = jnp.einsum(
        "nihgd,njhd->nhgij", q_blocks, keys_pair, preferred_element_type=jnp.float32
    ) * HEAD_DIM ** (-0.5)
    query_pos = anchor + (jnp.arange(blocks) * WINDOW)[:, None] + jnp.arange(WINDOW)[None, :]
    key_pos = (
        anchor + (jnp.arange(blocks) * WINDOW - WINDOW)[:, None] + jnp.arange(2 * WINDOW)[None, :]
    )
    allowed = (
        (key_pos[:, None, :] >= 0)
        & (key_pos[:, None, :] <= query_pos[:, :, None])
        & (query_pos[:, :, None] - key_pos[:, None, :] < WINDOW)
    )
    scores = jnp.where(allowed[:, None, None], scores, masked_out)
    sink_logit = sink_logits.reshape(kv_here, group_size)[None, :, :, None]
    highest = jnp.maximum(jnp.max(scores, axis=-1), sink_logit)
    lifted = jnp.exp(scores - highest[..., None])
    denominator = jnp.sum(lifted, axis=-1) + jnp.exp(sink_logit - highest)
    attn_weights = (lifted / denominator[..., None]).astype(jnp.bfloat16)
    final_product = jnp.einsum(
        "nhgij,njhd->nihgd", attn_weights, values_pair, preferred_element_type=jnp.float32
    )
    return final_product.reshape(tok_count, kv_here * group_size * HEAD_DIM).astype(jnp.bfloat16)


def ring_spot(index, count):
    half = count // 2
    return jnp.where(lax.rem(index, 2) == 0, index // 2, count - 1 - index // 2)


def ring_member(spot, count):
    half = count // 2
    return jnp.where(spot < half, 2 * spot, 2 * (count - 1 - spot) + 1)


def project_kernel(n, n_tp, normed_ref, pack_ref, log_ref, out_ref, logs_ref, rows_ref, held, total, sems, tok_sems):
    sp, tp = lax.axis_index("sp"), lax.axis_index("tp")
    depth, width = pack_ref.shape
    count = normed_ref.shape[0]
    half = n // 2
    spot = ring_spot(sp, n)
    ahead = ring_member(lax.rem(spot + 1, n), n)
    behind = ring_member(lax.rem(spot + n - 1, n), n)

    barrier = pltpu.get_barrier_semaphore()
    for peer in (ahead, behind):
        pl.semaphore_signal(barrier, inc=1, device_id=(peer, tp), device_id_type=MESH)
    for step in range(1, n_tp):
        pl.semaphore_signal(
            barrier, inc=1, device_id=(sp, lax.rem(tp + step, n_tp)), device_id_type=MESH
        )
    pl.semaphore_wait(barrier, 2 + n_tp - 1)

    def rows_of(member):
        return pl.ds(pl.multiple_of(member * depth, depth), depth)

    middle = (width // LANES + 1) // 2 * LANES
    spans = (pl.ds(0, middle), pl.ds(middle, width - middle))

    def owner(direction, distance):
        shift = n - distance if direction == 0 else distance
        return ring_member(lax.rem(spot + shift, n), n)

    def send(direction, step, part):
        member = owner(direction, step - 1)
        if part == 2:
            return pltpu.make_async_remote_copy(
                src_ref=log_ref if step == 1 else logs_ref.at[member],
                dst_ref=logs_ref.at[member],
                send_sem=sems.at[0, direction, step - 1, part],
                recv_sem=sems.at[1, direction, step - 1, part],
                device_id=(ahead if direction == 0 else behind, tp),
                device_id_type=MESH,
            )
        source = pack_ref.at[:, spans[part]] if step == 1 else held.at[rows_of(member), spans[part]]
        return pltpu.make_async_remote_copy(
            src_ref=source,
            dst_ref=held.at[rows_of(member), spans[part]],
            send_sem=sems.at[0, direction, step - 1, part],
            recv_sem=sems.at[1, direction, step - 1, part],
            device_id=(ahead if direction == 0 else behind, tp),
            device_id_type=MESH,
        )

    def arrival(direction, step, part):
        member = owner(direction, step)
        if part == 2:
            return pltpu.make_async_remote_copy(
                src_ref=log_ref,
                dst_ref=logs_ref.at[member],
                send_sem=sems.at[0, direction, step - 1, part],
                recv_sem=sems.at[1, direction, step - 1, part],
                device_id=(ahead if direction == 0 else behind, tp),
                device_id_type=MESH,
            )
        return pltpu.make_async_remote_copy(
            src_ref=held.at[rows_of(member), spans[part]],
            dst_ref=held.at[rows_of(member), spans[part]],
            send_sem=sems.at[0, direction, step - 1, part],
            recv_sem=sems.at[1, direction, step - 1, part],
            device_id=(ahead if direction == 0 else behind, tp),
            device_id_type=MESH,
        )

    started = []

    def go(copy):
        copy.start()
        started.append(copy)

    def parts_of(step, direction):
        first = direction
        if step == half:
            return (2, first) if direction == 0 else (first,)
        return (2, first, 1 - first)

    for slot in range(3):
        for direction in range(2):
            parts = parts_of(1, direction)
            if slot < len(parts):
                go(send(direction, 1, parts[slot]))
    tok_here = pl.ds(pl.multiple_of(tp * count, count), count)
    for step in range(1, n_tp):
        go(
            pltpu.make_async_remote_copy(
                src_ref=normed_ref,
                dst_ref=rows_ref.at[tok_here],
                send_sem=tok_sems.at[0, step - 1],
                recv_sem=tok_sems.at[1, step - 1],
                device_id=(sp, lax.rem(tp + step, n_tp)),
                device_id_type=MESH,
            )
        )
    rows_ref[tok_here, :] = normed_ref[...]
    logs_ref[sp] = log_ref[...]
    for step in range(1, n_tp):
        origin = pl.ds(pl.multiple_of(lax.rem(tp + n_tp - step, n_tp) * count, count), count)
        pltpu.make_async_remote_copy(
            src_ref=normed_ref,
            dst_ref=rows_ref.at[origin],
            send_sem=tok_sems.at[0, step - 1],
            recv_sem=tok_sems.at[1, step - 1],
            device_id=(sp, lax.rem(tp + step, n_tp)),
            device_id_type=MESH,
        ).wait_recv()

    blockwise = depth % LANES == 0

    def add(member, weights, first=False):
        columns = pl.ds(pl.multiple_of(member * depth, depth), depth)
        product = jnp.dot(rows_ref[:, columns], weights, preferred_element_type=jnp.float32)
        total[...] = product if first else total[...] + product

    if blockwise:
        add(sp, pack_ref[...], True)
    else:
        held[rows_of(sp), :] = pack_ref[...]
    for step in range(1, half + 1):
        for slot in range(3):
            for direction in range(2):
                parts = parts_of(step, direction)
                if slot < len(parts):
                    arrival(direction, step, parts[slot]).wait_recv()
                    if step < half and parts[slot] in parts_of(step + 1, direction):
                        go(send(direction, step + 1, parts[slot]))
        if blockwise:
            for direction in range(1 if step == half else 2):
                member = owner(direction, step)
                add(member, held[rows_of(member), :])
    if not blockwise:
        total[...] = jnp.dot(rows_ref[...], held[...], preferred_element_type=jnp.float32)
    out_ref[...] = total[...].astype(out_ref.dtype)
    for copy in started:
        copy.wait_send()


def project(normed, pack, logs, n, n_tp):
    depth, width = pack.shape
    count = normed.shape[0]
    features = normed.shape[1]
    vmem = pl.BlockSpec(memory_space=pltpu.VMEM)
    return pl.pallas_call(
        functools.partial(project_kernel, n, n_tp),
        out_shape=(
            jax.ShapeDtypeStruct((n_tp * count, width), jnp.bfloat16),
            jax.ShapeDtypeStruct((n,) + logs.shape, jnp.float32),
        ),
        in_specs=[vmem, vmem, vmem],
        out_specs=(vmem, vmem),
        scratch_shapes=[
            pltpu.VMEM((n_tp * count, features), jnp.bfloat16),
            pltpu.VMEM((n * depth, width), jnp.bfloat16),
            pltpu.VMEM((n_tp * count, width), jnp.float32),
            pltpu.SemaphoreType.DMA((2, 2, n // 2, 3)),
            pltpu.SemaphoreType.DMA((2, n_tp - 1)),
        ],
        compiler_params=pltpu.CompilerParams(
            collective_id=0, has_side_effects=True, vmem_limit_bytes=40 * 2**20
        ),
        cost_estimate=pl.CostEstimate(
            flops=400 * 2**30, bytes_accessed=n * depth * width * 2, transcendentals=0
        ),
        name="project_ring",
    )(normed, pack, logs)


def exchange_kernel(n, extra, rim_ref, state_ref, *refs):
    weight_refs = refs[:extra]
    before_ref, states_ref = refs[extra : extra + 2]
    whole_refs = refs[extra + 2 : 2 * extra + 2]
    sems, rim_sems = refs[2 * extra + 2 :]
    sources = [state_ref.at[0], state_ref.at[1], *weight_refs]
    sp, tp = lax.axis_index("sp"), lax.axis_index("tp")
    half = n // 2
    spot = ring_spot(sp, n)
    ahead = ring_member(lax.rem(spot + 1, n), n)
    behind = ring_member(lax.rem(spot + n - 1, n), n)
    later, earlier = lax.rem(sp + 1, n), lax.rem(sp + n - 1, n)
    barrier = pltpu.get_barrier_semaphore()
    for peer in (ahead, behind, later, earlier):
        pl.semaphore_signal(barrier, inc=1, device_id=(peer, tp), device_id_type=MESH)
    pl.semaphore_wait(barrier, 4)

    def owner(direction, distance):
        shift = n - distance if direction == 0 else distance
        return ring_member(lax.rem(spot + shift, n), n)

    def parts_of(step, direction):
        order = []
        for first in range(0, 2 + extra, 2):
            order.append(first + direction)
            if step < half:
                order.append(first + 1 - direction)
        return order

    def target(member, part):
        return states_ref.at[member, part] if part < 2 else whole_refs[part - 2].at[member]

    def hop(direction, step, part, member, source):
        return pltpu.make_async_remote_copy(
            src_ref=source,
            dst_ref=target(member, part),
            send_sem=sems.at[0, direction, step - 1, part],
            recv_sem=sems.at[1, direction, step - 1, part],
            device_id=(ahead if direction == 0 else behind, tp),
            device_id_type=MESH,
        )

    started = []
    rim = pltpu.make_async_remote_copy(
        src_ref=rim_ref,
        dst_ref=before_ref,
        send_sem=rim_sems.at[0],
        recv_sem=rim_sems.at[1],
        device_id=(later, tp),
        device_id_type=MESH,
    )
    for slot in range(2 + extra):
        for direction in range(2):
            parts = parts_of(1, direction)
            if slot < len(parts):
                copy = hop(direction, 1, parts[slot], sp, sources[parts[slot]])
                copy.start()
                started.append(copy)
    rim.start()
    states_ref[sp] = state_ref[...]
    for whole, piece in zip(whole_refs, weight_refs):
        whole[sp] = piece[...]
    for step in range(1, half + 1):
        for slot in range(2 + extra):
            for direction in range(2):
                parts = parts_of(step, direction)
                if slot < len(parts):
                    part = parts[slot]
                    member = owner(direction, step)
                    hop(direction, step, part, member, sources[part]).wait_recv()
                    if step < half and part in parts_of(step + 1, direction):
                        copy = hop(direction, step + 1, part, member, target(member, part))
                        copy.start()
                        started.append(copy)
    rim.wait()
    for copy in started:
        copy.wait_send()


def exchange(rim, state, weights, n):
    vmem = pl.BlockSpec(memory_space=pltpu.VMEM)
    return pl.pallas_call(
        functools.partial(exchange_kernel, n, len(weights)),
        out_shape=(
            jax.ShapeDtypeStruct(rim.shape, rim.dtype),
            jax.ShapeDtypeStruct((n,) + state.shape, state.dtype),
            *[jax.ShapeDtypeStruct((n,) + weight.shape, weight.dtype) for weight in weights],
        ),
        in_specs=[vmem] * (2 + len(weights)),
        out_specs=(vmem,) * (2 + len(weights)),
        scratch_shapes=[
            pltpu.SemaphoreType.DMA((2, 2, n // 2, 2 + len(weights))),
            pltpu.SemaphoreType.DMA((2,)),
        ],
        compiler_params=pltpu.CompilerParams(
            collective_id=2, has_side_effects=True, vmem_limit_bytes=40 * 2**20
        ),
        cost_estimate=pl.CostEstimate(
            flops=20 * 2**30, bytes_accessed=n * state.size * 2, transcendentals=0
        ),
        name="state_ring",
    )(rim, state, *weights)


def merge_kernel(n_tp, ret_ref, att_ref, ret_out_ref, att_out_ref, out_ref, total, outgoing, incoming, sent, landed, sems):
    sp, tp = lax.axis_index("sp"), lax.axis_index("tp")
    outer, inner = tp // 2, lax.rem(tp, 2)
    groups = n_tp // 2
    count = out_ref.shape[0]
    barrier = pltpu.get_barrier_semaphore()
    mate = outer * 2 + 1 - inner
    pl.semaphore_signal(barrier, inc=1, device_id=(sp, mate), device_id_type=MESH)
    for step in range(1, groups):
        peer = lax.rem(outer + step, groups) * 2 + inner
        pl.semaphore_signal(barrier, inc=1, device_id=(sp, peer), device_id_type=MESH)
    pl.semaphore_wait(barrier, groups)

    blocks, _, width = ret_out_ref.shape

    def partial(side, block):
        return jnp.dot(
            ret_ref[side], ret_out_ref[block], preferred_element_type=jnp.float32
        ) + jnp.dot(att_ref[side], att_out_ref[block], preferred_element_type=jnp.float32)

    for block in range(blocks):
        outgoing[:, block * width : (block + 1) * width] = partial(1 - inner, block).astype(
            jnp.bfloat16
        )
    swap = pltpu.make_async_remote_copy(
        src_ref=outgoing,
        dst_ref=incoming,
        send_sem=sems.at[0, 0],
        recv_sem=sems.at[1, 0],
        device_id=(sp, mate),
        device_id_type=MESH,
    )
    swap.start()
    for block in range(blocks):
        total[:, block * width : (block + 1) * width] = partial(inner, block)
    swap.wait_recv()
    own = total[...] + incoming[...].astype(jnp.float32)
    sent[...] = own.astype(jnp.bfloat16)
    copies = []
    for step in range(1, groups):
        other = lax.rem(outer + step, groups)
        copy = pltpu.make_async_remote_copy(
            src_ref=sent.at[pl.ds(pl.multiple_of(other * count, count), count)],
            dst_ref=landed.at[step - 1],
            send_sem=sems.at[0, step],
            recv_sem=sems.at[1, step],
            device_id=(sp, other * 2 + inner),
            device_id_type=MESH,
        )
        copy.start()
        copies.append(copy)
    mine = sent[pl.ds(pl.multiple_of(outer * count, count), count), :].astype(jnp.float32)
    for step, copy in enumerate(copies):
        copy.wait_recv()
        mine = mine + landed[step].astype(jnp.float32)
    out_ref[...] = mine.astype(out_ref.dtype)
    swap.wait_send()
    for copy in copies:
        copy.wait_send()


def merge(mixes, weights, n_tp):
    rows = mixes[0].shape[0]
    groups = n_tp // 2
    count = rows // n_tp
    width = weights[0].shape[0] * weights[0].shape[2]
    mixes = [
        mix.reshape(groups, 2, count, -1).transpose(1, 0, 2, 3).reshape(2, groups * count, -1)
        for mix in mixes
    ]
    vmem = pl.BlockSpec(memory_space=pltpu.VMEM)
    return pl.pallas_call(
        functools.partial(merge_kernel, n_tp),
        out_shape=jax.ShapeDtypeStruct((count, width), jnp.bfloat16),
        in_specs=[vmem] * 4,
        out_specs=vmem,
        scratch_shapes=[
            pltpu.VMEM((groups * count, width), jnp.float32),
            pltpu.VMEM((groups * count, width), jnp.bfloat16),
            pltpu.VMEM((groups * count, width), jnp.bfloat16),
            pltpu.VMEM((groups * count, width), jnp.bfloat16),
            pltpu.VMEM((max(1, groups - 1), count, width), jnp.bfloat16),
            pltpu.SemaphoreType.DMA((2, groups)),
        ],
        compiler_params=pltpu.CompilerParams(
            collective_id=1, has_side_effects=True, vmem_limit_bytes=40 * 2**20
        ),
        cost_estimate=pl.CostEstimate(
            flops=4 * rows * weights[0].size // 1, bytes_accessed=4 * weights[0].size, transcendentals=0
        ),
        name="merge_scatter",
    )(*mixes, *weights)


def on_device(
    tokens,
    norm_gain,
    ret_query,
    ret_key,
    ret_value,
    log_decay,
    att_query,
    att_key,
    att_value,
    sink_logits,
    ret_out,
    att_out,
):
    tok_float = tokens.astype(jnp.float32)
    normed = (
        tok_float
        * lax.rsqrt(jnp.mean(tok_float * tok_float, axis=-1, keepdims=True) + epsilon)
        * norm_gain
    ).astype(jnp.bfloat16)
    n, n_tp = lax.axis_size("sp"), lax.axis_size("tp")
    weights = (ret_query, ret_key, ret_value, att_query, att_key, att_value)
    widths = [weight.shape[1] for weight in weights]
    points = [sum(widths[:index]) for index in range(1, len(widths))]
    aligned = ret_out.shape[1] % LANES == 0
    local_logs = jnp.sum(log_decay, axis=1)
    log_tile = jnp.broadcast_to(
        jnp.pad(local_logs, (0, -local_logs.shape[0] % 8))[:, None], (-(-local_logs.shape[0] // 8) * 8, LANES)
    )
    projected, logs = project(normed, jnp.concatenate(weights, axis=1), log_tile, n, n_tp)
    logs = logs[:, : local_logs.shape[0], 0]
    sections = jnp.split(projected, points, axis=1)
    tok_count = sections[0].shape[0]
    anchor = lax.axis_index("sp") * tok_count
    positions = anchor + jnp.arange(tok_count, dtype=jnp.int32)
    query_ret = rotate(sections[0].reshape(tok_count, -1, RETAIN_KEY_SIZE), positions).astype(
        jnp.bfloat16
    )
    key_ret = (
        rotate(sections[1].reshape(tok_count, -1, RETAIN_KEY_SIZE), positions)
        * RETAIN_KEY_SIZE ** (-0.5)
    ).astype(jnp.bfloat16)
    value_ret = sections[2].reshape(tok_count, -1, V_DIM)
    stacked = projected[:, points[3] :]
    ret_mix, rim, wholes = retention_path(
        query_ret,
        key_ret,
        value_ret,
        log_decay,
        stacked[tok_count - WINDOW :],
        logs,
        (ret_out, att_out) if aligned else (),
    )
    if not aligned:
        wholes = [
            lax.all_gather(weight, "sp", axis=1, tiled=True)[None] for weight in (ret_out, att_out)
        ]
    att_mix = attention_path(sections[3], stacked, rim, sink_logits, anchor)
    return merge((ret_mix, att_mix), wholes, n_tp)


def solution(mesh):
    in_specs = (
        P(("sp", "tp"), None),
        P(),
        P("sp", "tp"),
        P("sp", "tp"),
        P("sp", "tp"),
        P("tp", "sp"),
        P("sp", "tp"),
        P("sp", "tp"),
        P("sp", "tp"),
        P("tp"),
        P("tp", "sp"),
        P("tp", "sp"),
    )
    out_specs = P(("sp", "tp"), None)
    return jax.shard_map(
        on_device, mesh=mesh, in_specs=in_specs, out_specs=out_specs, check_vma=False
    )
```
